256 devices in a mesh: ep: 16 (over y, x), tp: 16 (over z, core).
Axes of the slice: x: 4, y: 4, z: 8, core: 2. Of those that a mesh axis runs over, the one named last changes fastest.
Arguments:
- stream: bfloat16 [256, 2048], P('ep'), may hold values from -6 to 6
- norm_gain_attn: float32 [2048], replicated, may hold values from 0.1 to 1.9
- w_query: bfloat16 [2048, 2048], P('ep', 'tp'), may hold values from -0.125 to 0.125
- w_key: bfloat16 [2048, 2048], P('ep', 'tp'), may hold values from -0.125 to 0.125
- w_value: bfloat16 [2048, 2048], P('ep', 'tp'), may hold values from -0.125 to 0.125
- w_forget: bfloat16 [2048, 16], replicated, may hold values from -0.125 to 0.125
- forget_bias: float32 [16], replicated, may hold values from -2 to 2
- key_cache: bfloat16 [256, 1024, 2048], P('ep', None, 'tp'), may hold values from -1500 to 1500
- value_cache: bfloat16 [256, 1024, 2048], P('ep', None, 'tp'), may hold values from -6 to 6
- gate_cache: float32 [256, 16, 1024], P('ep', 'tp'), may hold values from -1024 to 0, as said below
- lengths: int32 [256], P('ep'), may hold values from 128 to 1024
- w_output: bfloat16 [2048, 2048], P('tp'), may hold values from -0.125 to 0.125
- norm_gain_ffn: float32 [2048], replicated, may hold values from 0.1 to 1.9
- routes: int32 [256, 2], replicated, may hold values from 0 to 15, all different within a row; in each aligned block of 16 rows (0 to 15, 16 to 31, ...) at most 4 rows name the same one
- route_weights: float32 [256, 2], replicated, may hold values from 0.2 to 1
- w_expert_gate: bfloat16 [16, 2048, 5632], P('ep', None, 'tp'), may hold values from -0.125 to 0.125
- w_expert_up: bfloat16 [16, 2048, 5632], P('ep', None, 'tp'), may hold values from -0.125 to 0.125
- expert_down_weight: bfloat16 [16, 5632, 2048], P('ep', 'tp'), may hold values from -0.078125 to 0.078125
Outputs:
- result: bfloat16 [256, 2048], P('ep', 'tp')
The draws below stay inside these ranges and needn't reach their ends.
Inputs may be any that keep to these rules, and one draw needn't show every extreme that they name: `gate_cache`: never rises along positions. `routes`: in the rows of one index of ep no expert is named by more than 4 rows, and in some such block one is named by exactly 4.
All inputs are finite; a program needn't handle non-finite values.
Results may differ from the reference program's by a relative error of at most 0.014.
Values may be sent and summed in bfloat16 or wider, within the bound.
A program may use at most 64 MiB of HBM per device.

```python
import math
import jax
import jax.numpy as jnp
import numpy as np
from jax import lax

D = 2048
HEADS = 16
HEAD_DIM = 128
FF = 5632
TOP = 2
SEQ_DEV = 16
CACHE = 1024
ATT = 2048
BATCH = 256
EXPERTS = 16
CAP = 4
N_EP = 16


def draw_key_cache(key, part):
    parts = jax.random.split(jax.random.fold_in(key, 11), 1)
    base = jax.random.normal(parts[0], (BATCH, CACHE, HEADS, HEAD_DIM), jnp.float32)
    return base.reshape(BATCH, CACHE, HEADS * HEAD_DIM).astype(jnp.bfloat16)


def draw_gate_cache(key, part):
    parts = jax.random.split(jax.random.fold_in(key, 23), 7)
    order = jax.random.permutation(parts[0], HEADS)
    fast_count = HEADS // 2
    fast = (order < fast_count)[None, :, None]
    block_factor = jnp.exp(jax.random.uniform(parts[1], (N_EP, 1, 1), jnp.float32, 0.0, math.log(4.0)))
    seq_factor = jnp.repeat(block_factor, SEQ_DEV, axis=0)
    fast_rate = jnp.exp(jax.random.uniform(parts[2], (BATCH, HEADS, 1), jnp.float32, math.log(1.0 / 50.0), math.log(1.0 / 30.0)))
    slow_rate = jnp.exp(jax.random.uniform(parts[3], (BATCH, HEADS, 1), jnp.float32, math.log(0.5), math.log(1.5))) / CACHE
    rate = jnp.where(fast, fast_rate, slow_rate) * seq_factor
    rough = jax.random.uniform(parts[4], (BATCH, HEADS, CACHE), jnp.float32, 0.0, 2.0)
    generation_iterations = -rate * rough
    sampled_locations = jax.random.randint(parts[5], (BATCH, HEADS, 3), 0, CACHE)
    stack_count = jax.random.uniform(parts[6], (BATCH, HEADS, 3), jnp.float32, math.log(0.5), math.log(0.8))
    sequence_indices = jnp.arange(CACHE)[None, None, None, :]
    clustered_sets = jnp.sum(jnp.where(sequence_indices == sampled_locations[..., None], stack_count[..., None], 0.0), axis=2)
    return jnp.cumsum(generation_iterations + clustered_sets, axis=2)


def touch_ends(drawn, rng, low, high):
    longest = drawn.shape.index(max(drawn.shape))
    spots = []
    for shift in (0, 1):
        where = [jax.random.randint(jax.random.fold_in(rng, axis), (), 0, length) for axis, length in enumerate(drawn.shape)]
        where[longest] = (where[longest] + shift) % drawn.shape[longest]
        spots.append(tuple(where))
    return drawn.at[spots[0]].set(low).at[spots[1]].set(high)


def level_of(own_key, shape, cuts, smallest, high):
    level = 1.0
    for position, blocks in cuts:
        heights = jax.random.uniform(jax.random.fold_in(jax.random.fold_in(own_key, 6), position), (blocks,), jnp.float32, smallest / len(cuts), high / len(cuts))
        level = level * jnp.repeat(jnp.exp(heights), shape[position] // blocks).reshape((-1,) + (1,) * (len(shape) - 1 - position))
    return level


def shared_out(own_key, own, number, rows, amount, top, bound, slope):
    sequence = jax.random.permutation(own_key, amount)
    packed, ordinary = shares(amount, rows * top, bound, slope, True), shares(amount, rows * top, bound, slope, False)
    places = jnp.arange(amount)

    def named(tallies, rotation):
        used = int((tallies > 0).sum())
        fixed = max(1, used // 4)
        moved = fixed + (places - fixed + rotation * (used - fixed)) % max(1, amount - fixed)
        return jnp.zeros((amount,), jnp.int32).at[sequence[jnp.where(places < fixed, places, moved)]].set(jnp.asarray(tallies, jnp.int32))

    tallies = jnp.where(number % 4 == 0, named(packed, number // 4), named(ordinary, number - number // 4 - 1))
    mixed = jax.random.permutation(jax.random.fold_in(own, 3), amount)
    donor, taker = mixed[0:amount // 2 * 2:2], mixed[1:amount // 2 * 2:2]
    margin = jnp.minimum(tallies[donor] - 1, bound - tallies[taker]) // 2
    margin = jnp.where((donor == sequence[0]) | (taker == sequence[0]) | (tallies[taker] == 0), 0, jnp.maximum(margin, 0))
    moved = jax.random.randint(jax.random.fold_in(own, 4), (amount // 2,), 0, 1 << 20) % (margin + 1)
    tallies = tallies.at[donor].add(-moved).at[taker].add(moved)
    items = jnp.searchsorted(jnp.cumsum(tallies), jnp.arange(rows * top), side="right").astype(jnp.int32)
    listing = items.reshape(top, rows).T
    listing = listing[jax.random.permutation(jax.random.fold_in(own, 1), rows)]
    rotation = jax.random.randint(jax.random.fold_in(own, 2), (rows, 1), 0, top)
    return jnp.take_along_axis(listing, (jnp.arange(top)[None, :] + rotation) % top, axis=1)


def shares(number_of, total, most, lean, full):
    portions = [(1 << 20) // math.isqrt(grade ** lean) + 1 for grade in range(1, number_of + 1)]
    largest = most if full else min(most, max(-(-total // number_of), total * portions[0] // sum(portions)))
    least = 1 if total - largest >= number_of - 1 else 0
    counts, spare = [largest] + [least] * (number_of - 1), total - largest - least * (number_of - 1)
    while spare > 0:
        movable = [i for i in range(1, number_of) if counts[i] < largest] or [i for i in range(1, number_of) if counts[i] < most]
        mass, remaining = sum([portions[i] for i in movable]), spare
        for i in movable:
            extra = min(most - counts[i], max(1, remaining * portions[i] // mass), spare)
            counts[i] = counts[i] + extra
            spare = spare - extra
    return np.array(counts)


def scatter_about(own_key, shape, spread, reach, cuts=(), held_as=jnp.bfloat16):
    result = spread * jax.random.normal(own_key, shape, jnp.float32)
    if cuts:
        result = result * level_of(own_key, shape, cuts, -0.22, 0.18)
    return jnp.clip(result, -reach, reach).astype(held_as)


def setup_inputs(seed: int = 0) -> dict:
    key_list = jax.random.split(jax.random.key(seed), 19)
    stream = scatter_about(key_list[0], (BATCH, D), 1.0, 6.0, ((0, 16),))
    norm_gain_attn = jnp.clip(1.0 + 0.18 * jax.random.normal(key_list[1], (D,), jnp.float32), 0.1, 1.9)
    w_query = scatter_about(key_list[2], (D, ATT), D ** -0.5, 0.125, ((0, 16), (1, 16)))
    w_key = scatter_about(key_list[3], (D, ATT), D ** -0.5, 0.125, ((0, 16), (1, 16)))
    w_value = scatter_about(key_list[4], (D, ATT), D ** -0.5, 0.125, ((0, 16), (1, 16)))
    w_forget = scatter_about(key_list[5], (D, HEADS), D ** -0.5, 0.125)
    forget_bias = jnp.clip(jax.random.uniform(key_list[6], (HEADS,), jnp.float32, -2.0, 2.0), -2.0, 2.0)
    key_cache = draw_key_cache(jax.random.fold_in(key_list[18], 71), 0)
    value_cache = scatter_about(key_list[8], (BATCH, CACHE, ATT), 1.0, 6.0, ((0, 16), (2, 16)))
    gate_cache = draw_gate_cache(jax.random.fold_in(key_list[18], 71), 0)
    lengths = touch_ends(jax.random.randint(key_list[10], (BATCH,), CACHE // 8, CACHE + 1), jax.random.fold_in(key_list[10], 1), CACHE // 8, CACHE).astype(jnp.int32)
    w_output = scatter_about(key_list[11], (ATT, D), ATT ** -0.5, 0.125, ((0, 16),))
    norm_gain_ffn = jnp.clip(1.0 + 0.18 * jax.random.normal(key_list[12], (D,), jnp.float32), 0.1, 1.9)
    routes_keys = jax.random.split(jax.random.fold_in(key_list[13], 1), BATCH // SEQ_DEV)
    routes_turns = jax.random.permutation(jax.random.fold_in(key_list[13], 3), BATCH // SEQ_DEV)
    routes = jax.vmap(lambda own, number: shared_out(jax.random.fold_in(key_list[13], 2), own, number, SEQ_DEV, EXPERTS, TOP, CAP, 2))(routes_keys, routes_turns).reshape((BATCH, TOP))
    route_weights = jnp.clip(jax.random.uniform(key_list[14], (BATCH, TOP), jnp.float32, 0.2, 1.0), 0.2, 1.0)
    w_expert_gate = scatter_about(key_list[15], (EXPERTS, D, FF), D ** -0.5, 0.125, ((0, 16), (2, 16)))
    w_expert_up = scatter_about(key_list[16], (EXPERTS, D, FF), D ** -0.5, 0.125, ((0, 16), (2, 16)))
    expert_down_weight = scatter_about(key_list[17], (EXPERTS, FF, D), FF ** -0.5, 0.078125, ((0, 16), (1, 16)))
    return dict(stream=stream, norm_gain_attn=norm_gain_attn, w_query=w_query, w_key=w_key, w_value=w_value, w_forget=w_forget, forget_bias=forget_bias, key_cache=key_cache, value_cache=value_cache, gate_cache=gate_cache, lengths=lengths, w_output=w_output, norm_gain_ffn=norm_gain_ffn, routes=routes, route_weights=route_weights, w_expert_gate=w_expert_gate, w_expert_up=w_expert_up, expert_down_weight=expert_down_weight)


def rms_norm(values, gain):
    floats = values.astype(jnp.float32)
    scaled = floats * lax.rsqrt(lax.optimization_barrier(jnp.mean(floats * floats, axis=-1, keepdims=True)) + 1e-06)
    return (scaled * gain).astype(jnp.bfloat16)

def attend_one(items):
    query, key_new, value_new, forget_new, keys, values, gates, length_total = items
    scale = HEAD_DIM ** (-0.5)
    query_f = query.astype(jnp.float32).reshape(HEADS, HEAD_DIM)
    keys_f = keys.astype(jnp.float32).reshape(CACHE, HEADS, HEAD_DIM)
    value_matrix_float = values.astype(jnp.float32).reshape(CACHE, HEADS, HEAD_DIM)
    sequence_indices = jnp.arange(CACHE, dtype=jnp.int32)
    is_live = sequence_indices < length_total
    last_gate = lax.optimization_barrier(jnp.sum(jnp.where(sequence_indices[None, :] == length_total - 1, gates, 0.0), axis=-1))
    scores = jnp.einsum('hd,phd->hp', query_f, keys_f) * scale + forget_new[:, None] + last_gate[:, None] - gates
    own_score = lax.optimization_barrier(jnp.sum(query_f * key_new.astype(jnp.float32).reshape(HEADS, HEAD_DIM), axis=-1)) * scale
    hidden_from_view = jnp.where(is_live[None, :], scores, -1e+30)
    largest = jnp.maximum(lax.optimization_barrier(jnp.max(hidden_from_view, axis=-1)), own_score)
    past = jnp.exp(hidden_from_view - largest[:, None])
    own_term = jnp.exp(own_score - largest)
    total = lax.optimization_barrier(jnp.sum(past, axis=-1)) + own_term
    past_weights = lax.optimization_barrier((past / total[:, None]).astype(jnp.bfloat16))
    own_weights = lax.optimization_barrier((own_term / total).astype(jnp.bfloat16))
    mixed = jnp.einsum('hp,phd->hd', past_weights.astype(jnp.float32), value_matrix_float)
    mixed = mixed + own_weights.astype(jnp.float32)[:, None] * value_new.astype(jnp.float32).reshape(HEADS, HEAD_DIM)
    return mixed.reshape(HEADS * HEAD_DIM).astype(jnp.bfloat16)

def reference(stream, norm_gain_attn, w_query, w_key, w_value, w_forget, forget_bias, key_cache, value_cache, gate_cache, lengths, w_output, norm_gain_ffn, routes, route_weights, w_expert_gate, w_expert_up, expert_down_weight):
    normed = rms_norm(stream, norm_gain_attn)
    query = jnp.dot(normed, w_query, preferred_element_type=jnp.float32).astype(jnp.bfloat16)
    key_new = jnp.dot(normed, w_key, preferred_element_type=jnp.float32).astype(jnp.bfloat16)
    value_new = jnp.dot(normed, w_value, preferred_element_type=jnp.float32).astype(jnp.bfloat16)
    forget_new = jax.nn.log_sigmoid(jnp.dot(normed, w_forget, preferred_element_type=jnp.float32) + forget_bias)
    attended = lax.map(attend_one, (query, key_new, value_new, forget_new, key_cache, value_cache, gate_cache, lengths))
    mixed = (stream.astype(jnp.float32) + jnp.dot(attended, w_output, preferred_element_type=jnp.float32)).astype(jnp.bfloat16)
    normed_ffn = rms_norm(mixed, norm_gain_ffn)
    flat_routes = routes.reshape(-1)
    flat_weights = route_weights.reshape(-1)
    owners = (jnp.arange(BATCH * TOP, dtype=jnp.int32) // TOP).astype(jnp.int32)
    slot_numbers = jnp.arange(CAP * N_EP, dtype=jnp.int32)

    def expert_step(combined, items):
        gate_w, up_w, down_w, index = items
        chosen = flat_routes == index
        chosen_count = jnp.sum(chosen.astype(jnp.int32))
        picks = jnp.nonzero(chosen, size=CAP * N_EP, fill_value=0)[0].astype(jnp.int32)
        token_ids = owners[picks]
        inputs = normed_ffn[token_ids]
        hidden = (jax.nn.silu(jnp.dot(inputs, gate_w, preferred_element_type=jnp.float32)) * jnp.dot(inputs, up_w, preferred_element_type=jnp.float32)).astype(jnp.bfloat16)
        outputs = lax.optimization_barrier(jnp.dot(hidden, down_w, preferred_element_type=jnp.float32).astype(jnp.bfloat16))
        weights = jnp.where(slot_numbers < chosen_count, flat_weights[picks], 0.0)
        return (combined.at[token_ids].add(outputs.astype(jnp.float32) * weights[:, None]), None)
    combined, _ = lax.scan(expert_step, jnp.zeros((BATCH, D), jnp.float32), (w_expert_gate, w_expert_up, expert_down_weight, jnp.arange(EXPERTS, dtype=jnp.int32)))
    return (mixed.astype(jnp.float32) + combined).astype(jnp.bfloat16)
```

```python
import functools

import jax
import jax.numpy as jnp
from jax import lax
from jax.experimental import pallas as pl
from jax.experimental.pallas import tpu as pltpu
from jax.sharding import PartitionSpec as P

MESH = pl.DeviceIdType.MESH
F32, BF16 = jnp.float32, jnp.bfloat16
NN = (((1,), (0,)), ((), ()))
NT = (((1,), (1,)), ((), ()))


def mm(a, b, dims=NN):
    return lax.dot_general(a, b, dims, preferred_element_type=F32)


def iota(shape, dim):
    return lax.broadcasted_iota(jnp.int32, shape, dim)


def ep_peer(me, i, n):
    if n != 16:
        return lax.rem(me + 1 + i, n)
    o = jnp.where(i < 11, 11 - i, 26 - i)
    y = lax.rem(me // 4 + o // 4, 4)
    x = lax.rem(lax.rem(me, 4) + lax.rem(o, 4), 4)
    return y * 4 + x


def tp_peer(me, i, n):
    half = (i + 1) // 2
    o = n // 2 + jnp.where(lax.rem(i, 2) == 1, -half, half)
    return lax.rem(me + o, n)


def kernel(
    cfg,
    stream_h, gain1_h, wq_h, wk_h, wv_h, wf_h, fb_h, kc_h, vc_h, gc_h, len_h,
    wo_h, gain2_h, rt_h, rw_h, wg_h, wu_h, wd_h,
    out_ref,
    stream, gain1, wqkv, wf, fb, kc, vc, gc, lens, wo, gain2, rt, rw, wg, wu, wd,
    xn, xin, qs, kvs, qr, kvr, os_, or_, mx, mxr, ss, sr, es, er, fs, fr,
    pick, unpick, spread, comb,
    load_sem, send_sem, recv_sem,
):
    ne, nt, cap = cfg
    seqs, width = stream.shape
    blk = width // ne
    slc = width // nt
    cache = kc.shape[1]
    hd = kc.shape[2]
    parts = 16 // cap
    cw = width // parts
    g = lax.axis_index("ep")
    t = lax.axis_index("tp")

    barrier = pltpu.get_barrier_semaphore()

    def greet_ep(i, c):
        pl.semaphore_signal(barrier, inc=1, device_id={"ep": ep_peer(g, i, ne)}, device_id_type=MESH)
        return c

    def greet_tp(i, c):
        pl.semaphore_signal(barrier, inc=1, device_id={"tp": tp_peer(t, i, nt)}, device_id_type=MESH)
        return c

    lax.fori_loop(0, ne - 1, greet_ep, 0)
    lax.fori_loop(0, nt - 1, greet_tp, 0)

    loads = [
        (stream_h, stream), (gain1_h, gain1),
        (wq_h, wqkv.at[:, pl.ds(0, hd)]), (wk_h, wqkv.at[:, pl.ds(hd, hd)]),
        (wv_h, wqkv.at[:, pl.ds(2 * hd, hd)]),
        (wf_h, wf), (fb_h, fb), (len_h, lens), (rt_h, rt), (rw_h, rw), (gc_h, gc),
        (kc_h, kc), (wo_h, wo), (vc_h, vc), (gain2_h, gain2),
        (wg_h.at[0], wg), (wu_h.at[0], wu), (wd_h.at[0], wd),
    ]
    copies = [pltpu.make_async_copy(a, b, load_sem.at[i]) for i, (a, b) in enumerate(loads)]
    for c in copies:
        c.start()
    (c_stream, c_gain1, c_q, c_k, c_v, c_wf, c_fb, c_len, c_rt, c_rw, c_gc,
     c_kc, c_wo, c_vc, c_gain2, c_wg, c_wu, c_wd) = copies

    def remote(src, dst, phase, where):
        return pltpu.make_async_remote_copy(
            src_ref=src, dst_ref=dst, send_sem=send_sem.at[phase], recv_sem=recv_sem.at[phase],
            device_id=where, device_id_type=MESH)

    def send_ep(pairs):
        def body(i, c):
            peer = ep_peer(g, i, ne)
            for src, dst, phase in pairs:
                remote(src.at[peer], dst.at[g], phase, {"ep": peer}).start()
            return c
        lax.fori_loop(0, ne - 1, body, 0)

    def send_tp(src, dst, phase, whole=False):
        def body(i, c):
            peer = tp_peer(t, i, nt)
            remote(src if whole else src.at[peer], dst.at[t], phase, {"tp": peer}).start()
            return c
        lax.fori_loop(0, nt - 1, body, 0)

    def arrived(buf, phase, axis, n):
        part = buf.at[pl.ds(0, n - 1)]
        remote(part, part, phase, {axis: 0}).wait_recv()

    def gone(buf, phase, axis, n):
        part = buf.at[pl.ds(0, n - 1)]
        remote(part, part, phase, {axis: 0}).wait_send()

    c_stream.wait()
    c_gain1.wait()
    xf = stream[...].astype(F32)
    rs = lax.rsqrt(jnp.mean(xf * xf, axis=-1, keepdims=True) + 1e-06)
    normed = (xf * rs * gain1[...]).astype(BF16)
    for b in range(ne):
        xn[b] = normed[:, b * blk:(b + 1) * blk]
    pl.semaphore_wait(barrier, ne + nt - 2)
    send_ep([(xn, xin, 0)])
    xin[g] = xn[g]

    c_wf.wait()
    c_fb.wait()
    fz = mm(normed, wf[...], NT) + fb[...]
    heads = fz.shape[1]
    z = jnp.sum(jnp.where(iota(fz.shape, 1) == t, fz, 0.0), axis=1, keepdims=True)
    forget = jnp.minimum(z, 0.0) - jnp.log1p(jnp.exp(-jnp.abs(z)))

    c_len.wait()
    lsq = iota((seqs, seqs), 0) == iota((seqs, seqs), 1)
    length = jnp.sum(jnp.where(lsq, lens[...].astype(F32), 0.0), axis=1, keepdims=True).astype(jnp.int32)
    c_gc.wait()
    row = iota((seqs, cache), 0)
    pos = iota((seqs, cache), 1)
    gates = jnp.zeros((seqs, cache), F32)
    for s in range(seqs):
        gates = jnp.where(row == s, gc[s], gates)
    live = pos < length
    last_gate = jnp.sum(jnp.where(pos == length - 1, gates, 0.0), axis=1, keepdims=True)

    c_rt.wait()
    c_rw.wait()
    batch = rt.shape[1]
    mine = iota((seqs, batch), 1) == g * seqs + iota((seqs, batch), 0)
    lanes = ne * 16
    lane = iota((seqs, lanes), 1)
    lane_e, lane_j, lane_r = lane // 16, lax.rem(lane // cap, parts), lax.rem(lane, cap)
    chosen = jnp.zeros((seqs, lanes), F32)
    weight = jnp.zeros((seqs, lanes), F32)
    for k in range(rt.shape[0]):
        rk = jnp.sum(jnp.where(mine, rt[k:k + 1, :].astype(F32), 0.0), axis=1, keepdims=True).astype(jnp.int32)
        wk_ = jnp.sum(jnp.where(mine, rw[k:k + 1, :], 0.0), axis=1, keepdims=True)
        hit = rk == lane_e
        chosen = chosen + jnp.where(hit, 1.0, 0.0)
        weight = weight + jnp.where(hit, wk_, 0.0)
    before = (iota((seqs, seqs), 1) < iota((seqs, seqs), 0)).astype(F32).astype(BF16)
    rank = mm(before, chosen.astype(BF16))
    slot = rank == lane_r.astype(F32)
    chosen = jnp.where(slot, chosen, 0.0)
    weight = jnp.where(slot, weight, 0.0)
    w_hi = weight.astype(BF16)
    w_lo = (weight - w_hi.astype(F32)).astype(BF16)
    picked = []
    for j in range(parts):
        here = lane_j == j
        picked.append(jnp.where(here, chosen, 0.0))
        zero = jnp.zeros_like(w_hi)
        comb[pl.ds(2 * j * seqs, seqs), :] = jnp.where(here, w_hi.astype(F32), 0.0).astype(BF16)
        comb[pl.ds((2 * j + 1) * seqs, seqs), :] = jnp.where(here, w_lo.astype(F32), 0.0).astype(BF16)
    pick[...] = jnp.concatenate(picked, axis=0).T.astype(BF16)

    rows = ne * cap
    a, b = iota((parts * rows, lanes), 0), iota((parts * rows, lanes), 1)
    same = (a // rows == lax.rem(b // cap, parts)) & (lax.rem(a, rows) // cap == b // 16) & (lax.rem(a, cap) == lax.rem(b, cap))
    unpick[...] = jnp.where(same, 1.0, 0.0).astype(BF16)
    a, b = iota((lanes, parts * rows), 1), iota((lanes, parts * rows), 0)
    same = (a // rows == lax.rem(b // cap, parts)) & (lax.rem(a, rows) // cap == b // 16) & (lax.rem(a, cap) == lax.rem(b, cap))
    spread[...] = jnp.where(same, 1.0, 0.0).astype(BF16)

    c_q.wait()
    c_k.wait()
    c_v.wait()
    arrived(xin, 0, "ep", ne)
    proj = mm(xin[...].reshape(ne * seqs, blk), wqkv[...])
    qs[...] = proj[:, :hd].reshape(ne, seqs, hd)
    kvs[...] = proj[:, hd:].astype(BF16).reshape(ne, seqs, 2 * hd)
    send_ep([(qs, qr, 1), (kvs, kvr, 2)])
    qr[g] = qs[g]
    kvr[g] = kvs[g]
    arrived(qr, 1, "ep", ne)
    arrived(kvr, 2, "ep", ne)
    query = jnp.sum(qr[...], axis=0).astype(BF16)
    kv = jnp.sum(kvr[...].astype(F32), axis=0).astype(BF16)
    key_new, value_new = kv[:, :hd], kv[:, hd:]

    scale = hd ** (-0.5)
    c_kc.wait()
    scores = jnp.zeros((seqs, cache), F32)
    for s in range(seqs):
        scores = jnp.where(row == s, mm(query, kc[s], NT), scores)
    scores = scores * scale + forget + last_gate - gates
    scores = jnp.where(live, scores, -1e30)
    own = jnp.sum(query.astype(F32) * key_new.astype(F32), axis=1, keepdims=True) * scale
    top = jnp.maximum(jnp.max(scores, axis=1, keepdims=True), own)
    past = jnp.exp(scores - top)
    own = jnp.exp(own - top)
    total = jnp.sum(past, axis=1, keepdims=True) + own
    past = (past / total).astype(BF16)
    own = (own / total).astype(BF16)
    c_vc.wait()
    hrow = iota((seqs, hd), 0)
    att = jnp.zeros((seqs, hd), F32)
    for s in range(seqs):
        att = jnp.where(hrow == s, mm(past, vc[s]), att)
    att = (att + own.astype(F32) * value_new.astype(F32)).astype(BF16)

    c_wo.wait()
    share = mm(att, wo[...]).astype(BF16)
    for u in range(nt):
        os_[u] = share[:, u * slc:(u + 1) * slc]
    send_tp(os_, or_, 3)
    or_[t] = os_[t]
    own_stream = stream[:, pl.ds(pl.multiple_of(t * slc, slc), slc)].astype(F32)
    arrived(or_, 3, "tp", nt)
    mixed = (own_stream + jnp.sum(or_[...].astype(F32), axis=0)).astype(BF16)
    mx[...] = mixed
    send_tp(mx, mxr, 4, whole=True)
    mxr[t] = mixed
    arrived(mxr, 4, "tp", nt)

    per = nt // parts
    stacked = jnp.concatenate(
        [jnp.concatenate([mxr[j * per + u] for u in range(per)], axis=1) for j in range(parts)], axis=0)
    ss[...] = mm(pick[...], stacked).astype(BF16).reshape(ne, 16, cw)
    send_ep([(ss, sr, 5)])
    sr[g] = ss[g]
    c_gain2.wait()
    c_wg.wait()
    c_wu.wait()
    arrived(sr, 5, "ep", ne)
    rows_in = mm(unpick[...], sr[...].reshape(lanes, cw))
    xs = jnp.concatenate([rows_in[j * rows:(j + 1) * rows] for j in range(parts)], axis=1)
    rs2 = lax.rsqrt(jnp.mean(xs * xs, axis=-1, keepdims=True) + 1e-06)
    xs = (xs * rs2 * gain2[...]).astype(BF16)
    gate = mm(xs, wg[...], NT)
    up = mm(xs, wu[...], NT)
    hidden = (gate / (1.0 + jnp.exp(-gate)) * up).astype(BF16)
    c_wd.wait()
    part = mm(hidden, wd[...]).astype(BF16)
    part = jnp.concatenate([part[:, j * cw:(j + 1) * cw] for j in range(parts)], axis=0)
    es[...] = mm(spread[...], part).astype(BF16).reshape(ne, 16, cw)
    send_ep([(es, er, 6)])
    er[g] = es[g]
    arrived(er, 6, "ep", ne)

    both = mm(comb[...], er[...].reshape(lanes, cw))
    for j in range(parts):
        piece = (both[2 * j * seqs:(2 * j + 1) * seqs] + both[(2 * j + 1) * seqs:(2 * j + 2) * seqs]).astype(BF16)
        for u in range(per):
            fs[j * per + u] = piece[:, u * slc:(u + 1) * slc]
    send_tp(fs, fr, 7)
    fr[t] = fs[t]
    arrived(fr, 7, "tp", nt)
    out_ref[...] = (mixed.astype(F32) + jnp.sum(fr[...].astype(F32), axis=0)).astype(BF16)

    for buf, phase, axis, n in (
        (xin, 0, "ep", ne), (qr, 1, "ep", ne), (kvr, 2, "ep", ne), (or_, 3, "tp", nt),
        (mxr, 4, "tp", nt), (sr, 5, "ep", ne), (er, 6, "ep", ne), (fr, 7, "tp", nt)):
        gone(buf, phase, axis, n)


def shards(
    ne, nt, stream, norm_gain_attn, w_query, w_key, w_value, w_forget, forget_bias,
    key_cache, value_cache, gate_cache, lengths, w_output, norm_gain_ffn,
    routes, route_weights, w_expert_gate, w_expert_up, expert_down_weight,
):
    seqs, width = stream.shape
    cache, hd = key_cache.shape[1:]
    tops = routes.shape[1]
    cap = 2 * seqs * tops // ne
    blk, slc, hid = width // ne, width // nt, w_expert_gate.shape[2]
    parts = 16 // cap
    cw = width // parts
    args = (
        stream, norm_gain_attn.reshape(1, -1), w_query, w_key, w_value, w_forget.T,
        forget_bias.reshape(1, -1), key_cache, value_cache, gate_cache, lengths.reshape(1, -1),
        w_output, norm_gain_ffn.reshape(1, -1), routes.T, route_weights.T,
        jnp.swapaxes(w_expert_gate, 1, 2), jnp.swapaxes(w_expert_up, 1, 2), expert_down_weight,
    )
    V = pltpu.VMEM
    scratch = [
        V((seqs, width), BF16), V((1, width), F32), V((blk, 3 * hd), BF16),
        V(w_forget.shape[::-1], BF16), V((1, forget_bias.shape[0]), F32),
        V(key_cache.shape, BF16), V(value_cache.shape, BF16), V(gate_cache.shape, F32),
        V((1, seqs), jnp.int32), V(w_output.shape, BF16), V((1, width), F32),
        V(routes.shape[::-1], jnp.int32), V(routes.shape[::-1], F32),
        V((hid, width), BF16), V((hid, width), BF16), V((hid, width), BF16),
        V((ne, seqs, blk), BF16), V((ne, seqs, blk), BF16),
        V((ne, seqs, hd), F32), V((ne, seqs, 2 * hd), BF16),
        V((ne, seqs, hd), F32), V((ne, seqs, 2 * hd), BF16),
        V((nt, seqs, slc), BF16), V((nt, seqs, slc), BF16),
        V((seqs, slc), BF16), V((nt, seqs, slc), BF16),
        V((ne, 16, cw), BF16), V((ne, 16, cw), BF16),
        V((ne, 16, cw), BF16), V((ne, 16, cw), BF16),
        V((nt, seqs, slc), BF16), V((nt, seqs, slc), BF16),
        V((ne * 16, parts * seqs), BF16), V((parts * ne * cap, ne * 16), BF16),
        V((ne * 16, parts * ne * cap), BF16), V((2 * parts * seqs, ne * 16), BF16),
        pltpu.SemaphoreType.DMA((18,)), pltpu.SemaphoreType.DMA((8,)), pltpu.SemaphoreType.DMA((8,)),
    ]
    return pl.pallas_call(
        functools.partial(kernel, (ne, nt, cap)),
        out_shape=jax.ShapeDtypeStruct((seqs, slc), BF16),
        in_specs=[pl.BlockSpec(memory_space=pl.ANY)] * len(args),
        out_specs=pl.BlockSpec(memory_space=pltpu.VMEM),
        scratch_shapes=scratch,
        compiler_params=pltpu.CompilerParams(
            collective_id=0, has_side_effects=True, vmem_limit_bytes=48 * 1024 * 1024),
        name="layer",
    )(*args)


def solution(mesh):
    placed = (
        P("ep", None), P(), P("ep", "tp"), P("ep", "tp"), P("ep", "tp"), P(), P(),
        P("ep", None, "tp"), P("ep", None, "tp"), P("ep", "tp", None), P("ep"),
        P("tp", None), P(), P(), P(),
        P("ep", None, "tp"), P("ep", None, "tp"), P("ep", "tp", None),
    )
    return jax.shard_map(
        functools.partial(shards, mesh.shape["ep"], mesh.shape["tp"]),
        mesh=mesh, in_specs=placed, out_specs=P("ep", "tp"), check_vma=False,
    )
```

```python
import functools

import jax
import jax.numpy as jnp
from jax import lax
from jax.experimental import pallas as pl
from jax.experimental.pallas import tpu as pltpu
from jax.sharding import PartitionSpec as P

MESH = pl.DeviceIdType.MESH
F32, BF16 = jnp.float32, jnp.bfloat16
NN = (((1,), (0,)), ((), ()))
NT = (((1,), (1,)), ((), ()))


def mm(a, b, dims=NN):
    return lax.dot_general(a, b, dims, preferred_element_type=F32)


def iota(shape, dim):
    return lax.broadcasted_iota(jnp.int32, shape, dim)


def ring(me, n, size=1):
    return [(min(o, n - o) * size, lax.rem(me + o, n)) for o in range(1, n)]


def plane(me, n):
    if n != 16:
        return [p for _, p in sorted(ring(me, n), key=lambda q: -q[0])]
    y, x = me // 4, lax.rem(me, 4)
    ys = [(0, y)] + ring(y, 4)
    xs = [(0, x)] + ring(x, 4)
    both = [(dy + dx, py * 4 + px) for dy, py in ys for dx, px in xs]
    return [p for _, p in sorted(both[1:], key=lambda q: -q[0])]


def kernel(
    cfg,
    stream_h, gain1_h, wq_h, wk_h, wv_h, wf_h, fb_h, kc_h, vc_h, gc_h, len_h,
    wo_h, gain2_h, rt_h, rw_h, wg_h, wu_h, wd_h,
    out_ref,
    stream, gain1, wqkv, wf, fb, kc, vc, gc, lens, wo, gain2, rt, rw, wgu, wd,
    xn, xin, qs, kvs, qr, kvr, os_, or_, mx, mxr, ss, sr, es, er, fs, fr,
    pick, unpick, spread, comb,
    load_sem, send_sem, recv_sem,
):
    ne, nt, cap = cfg
    seqs, width = stream.shape
    blk = width // ne
    slc = width // nt
    nz = nt // 2
    hid = wd.shape[0]
    cache = kc.shape[1]
    hd = kc.shape[2]
    parts = 16 // cap
    cw = width // 2 // parts
    g = lax.axis_index("ep")
    t = lax.axis_index("tp")
    z, core = t // 2, lax.rem(t, 2)

    loads = [
        (stream_h, stream), (gain1_h, gain1),
        (wq_h, wqkv.at[:, pl.ds(0, hd)]), (wk_h, wqkv.at[:, pl.ds(hd, hd)]),
        (wv_h, wqkv.at[:, pl.ds(2 * hd, hd)]),
        (wf_h, wf), (fb_h, fb), (len_h, lens), (rt_h, rt), (rw_h, rw), (gc_h, gc),
        (kc_h, kc), (wo_h, wo), (vc_h, vc), (gain2_h, gain2),
        (wg_h.at[0], wgu.at[pl.ds(0, hid)]), (wu_h.at[0], wgu.at[pl.ds(hid, hid)]), (wd_h.at[0], wd),
    ]
    copies = [pltpu.make_async_copy(a, b, load_sem.at[i]) for i, (a, b) in enumerate(loads)]
    copies[0].start()
    copies[1].start()

    barrier = pltpu.get_barrier_semaphore()

    far_ep = plane(g, ne)
    far_z = [p for _, p in sorted(ring(z, nz), key=lambda q: -q[0])]
    far_tp = [2 * p + k for p in far_z for k in range(2)] + [2 * z + 1 - core]
    for i in range(max(ne, nt) - 1):
        for axis, peers in (("ep", far_ep), ("tp", far_tp)):
            if i < len(peers):
                pl.semaphore_signal(barrier, inc=1, device_id={axis: peers[i]}, device_id_type=MESH)
    for c in copies[2:]:
        c.start()
    (c_stream, c_gain1, c_q, c_k, c_v, c_wf, c_fb, c_len, c_rt, c_rw, c_gc,
     c_kc, c_wo, c_vc, c_gain2, c_wg, c_wu, c_wd) = copies

    def remote(src, dst, phase, where):
        return pltpu.make_async_remote_copy(
            src_ref=src, dst_ref=dst, send_sem=send_sem.at[phase], recv_sem=recv_sem.at[phase],
            device_id=where, device_id_type=MESH)

    def send_ep(src, dst, phase):
        for peer in far_ep:
            remote(src.at[peer], dst.at[g], phase, {"ep": peer}).start()

    def send_tp(src, dst, phase):
        for peer in far_tp:
            remote(src.at[peer], dst.at[t], phase, {"tp": peer}).start()

    def send_z(src, dst, phase, whole=False):
        for peer in far_z:
            remote(src if whole else src.at[peer], dst.at[z], phase, {"tp": 2 * peer + core}).start()

    def send_chips(src, dst, phase, split):
        for peer in far_ep:
            for k in range(2):
                block = src.at[k * ne + peer] if split else src.at[peer]
                remote(block, dst.at[core * ne + g], phase, {"ep": peer, "tp": 2 * z + k}).start()
        other = (1 - core) * ne if split else 0
        remote(src.at[other + g], dst.at[core * ne + g], phase, {"tp": 2 * z + 1 - core}).start()

    def arrived(buf, phase):
        part = buf.at[pl.ds(0, buf.shape[0] - 1)]
        remote(part, part, phase, {"ep": 0}).wait_recv()

    def gone(buf, phase):
        part = buf.at[pl.ds(0, buf.shape[0] - 1)]
        remote(part, part, phase, {"ep": 0}).wait_send()

    c_stream.wait()
    c_gain1.wait()
    xf = stream[...].astype(F32)
    rs = lax.rsqrt(jnp.mean(xf * xf, axis=-1, keepdims=True) + 1e-06)
    normed = (xf * rs * gain1[...]).astype(BF16)
    for b in range(ne):
        xn[b] = normed[:, b * blk:(b + 1) * blk]
    pl.semaphore_wait(barrier, ne + nt - 2)
    send_ep(xn, xin, 0)
    xin[g] = xn[g]

    c_wf.wait()
    c_fb.wait()
    fz = mm(normed, wf[...], NT) + fb[...]
    fz = jnp.sum(jnp.where(iota(fz.shape, 1) == t, fz, 0.0), axis=1, keepdims=True)
    forget = jnp.minimum(fz, 0.0) - jnp.log1p(jnp.exp(-jnp.abs(fz)))

    c_len.wait()
    lsq = iota((seqs, seqs), 0) == iota((seqs, seqs), 1)
    length = jnp.sum(jnp.where(lsq, lens[...].astype(F32), 0.0), axis=1, keepdims=True).astype(jnp.int32)
    c_gc.wait()
    row = iota((seqs, cache), 0)
    pos = iota((seqs, cache), 1)
    gates = jnp.zeros((seqs, cache), F32)
    for s in range(seqs):
        gates = jnp.where(row == s, gc[s], gates)
    live = pos < length
    last_gate = jnp.sum(jnp.where(pos == length - 1, gates, 0.0), axis=1, keepdims=True)

    c_rt.wait()
    c_rw.wait()
    batch = rt.shape[1]
    mine = iota((seqs, batch), 1) == g * seqs + iota((seqs, batch), 0)
    lanes = ne * 16
    lane = iota((seqs, lanes), 1)
    lane_e, lane_j, lane_r = lane // 16, lax.rem(lane // cap, parts), lax.rem(lane, cap)
    chosen = jnp.zeros((seqs, lanes), F32)
    weight = jnp.zeros((seqs, lanes), F32)
    for k in range(rt.shape[0]):
        rk = jnp.sum(jnp.where(mine, rt[k:k + 1, :].astype(F32), 0.0), axis=1, keepdims=True).astype(jnp.int32)
        wk_ = jnp.sum(jnp.where(mine, rw[k:k + 1, :], 0.0), axis=1, keepdims=True)
        hit = rk == lane_e
        chosen = chosen + jnp.where(hit, 1.0, 0.0)
        weight = weight + jnp.where(hit, wk_, 0.0)
    before = (iota((seqs, seqs), 1) < iota((seqs, seqs), 0)).astype(F32).astype(BF16)
    rank = mm(before, chosen.astype(BF16))
    slot = rank == lane_r.astype(F32)
    chosen = jnp.where(slot, chosen, 0.0)
    weight = jnp.where(slot, weight, 0.0)
    w_hi = weight.astype(BF16)
    w_lo = (weight - w_hi.astype(F32)).astype(BF16)
    picked = []
    for j in range(parts):
        here = lane_j == j
        picked.append(jnp.where(here, chosen, 0.0))
        zero = jnp.zeros_like(w_hi)
        comb[pl.ds(2 * j * seqs, seqs), :] = jnp.where(here, w_hi.astype(F32), 0.0).astype(BF16)
        comb[pl.ds((2 * j + 1) * seqs, seqs), :] = jnp.where(here, w_lo.astype(F32), 0.0).astype(BF16)
    pick[...] = jnp.concatenate(picked, axis=0).T.astype(BF16)

    rows = ne * cap
    a, b = iota((parts * rows, lanes), 0), iota((parts * rows, lanes), 1)
    same = (a // rows == lax.rem(b // cap, parts)) & (lax.rem(a, rows) // cap == b // 16) & (lax.rem(a, cap) == lax.rem(b, cap))
    unpick[...] = jnp.where(same, 1.0, 0.0).astype(BF16)
    a, b = iota((lanes, parts * rows), 1), iota((lanes, parts * rows), 0)
    same = (a // rows == lax.rem(b // cap, parts)) & (lax.rem(a, rows) // cap == b // 16) & (lax.rem(a, cap) == lax.rem(b, cap))
    spread[...] = jnp.where(same, 1.0, 0.0).astype(BF16)

    c_q.wait()
    c_k.wait()
    c_v.wait()
    arrived(xin, 0)
    proj = mm(xin[...].reshape(ne * seqs, blk), wqkv[...])
    qs[...] = proj[:, :hd].reshape(ne, seqs, hd)
    kvs[...] = proj[:, hd:].astype(BF16).reshape(ne, seqs, 2 * hd)
    send_ep(qs, qr, 1)
    send_ep(kvs, kvr, 2)
    qr[g] = qs[g]
    kvr[g] = kvs[g]
    arrived(qr, 1)
    query = jnp.sum(qr[...], axis=0).astype(BF16)

    scale = hd ** (-0.5)
    c_kc.wait()
    scores = jnp.zeros((seqs, cache), F32)
    for s in range(seqs):
        scores = jnp.where(row == s, mm(query, kc[s], NT), scores)
    scores = scores * scale + forget + last_gate - gates
    scores = jnp.where(live, scores, -1e30)
    arrived(kvr, 2)
    kv = jnp.sum(kvr[...].astype(F32), axis=0).astype(BF16)
    key_new, value_new = kv[:, :hd], kv[:, hd:]
    own = jnp.sum(query.astype(F32) * key_new.astype(F32), axis=1, keepdims=True) * scale
    top = jnp.maximum(jnp.max(scores, axis=1, keepdims=True), own)
    past = jnp.exp(scores - top)
    own = jnp.exp(own - top)
    total = jnp.sum(past, axis=1, keepdims=True) + own
    past = (past / total).astype(BF16)
    own = (own / total).astype(BF16)
    c_vc.wait()
    hrow = iota((seqs, hd), 0)
    att = jnp.zeros((seqs, hd), F32)
    for s in range(seqs):
        att = jnp.where(hrow == s, mm(past, vc[s]), att)
    att = (att + own.astype(F32) * value_new.astype(F32)).astype(BF16)

    c_wo.wait()
    share = mm(att, wo[...]).astype(BF16)
    for u in range(nt):
        os_[u] = share[:, u * slc:(u + 1) * slc]
    send_tp(os_, or_, 3)
    or_[t] = os_[t]
    own_stream = stream[:, pl.ds(pl.multiple_of(t * slc, slc), slc)].astype(F32)
    arrived(or_, 3)
    mixed = (own_stream + jnp.sum(or_[...].astype(F32), axis=0)).astype(BF16)
    mx[...] = mixed
    send_z(mx, mxr, 4, whole=True)
    mxr[z] = mixed
    arrived(mxr, 4)

    per = nz // parts
    stacked = jnp.concatenate(
        [jnp.concatenate([mxr[j * per + u] for u in range(per)], axis=1) for j in range(parts)], axis=0)
    ss[...] = mm(pick[...], stacked).astype(BF16).reshape(ne, 16, cw)
    send_chips(ss, sr, 5, False)
    sr[core * ne + g] = ss[g]
    c_gain2.wait()
    c_wg.wait()
    c_wu.wait()
    arrived(sr, 5)
    halves = [mm(unpick[...], sr[pl.ds(k * ne, ne)].reshape(lanes, cw)) for k in range(2)]
    xs = []
    for u in range(nt):
        j, v = u // 2 // per, u // 2 % per
        xs.append(halves[u % 2][j * rows:(j + 1) * rows, v * slc:(v + 1) * slc])
    xs = jnp.concatenate(xs, axis=1)
    rs2 = lax.rsqrt(jnp.mean(xs * xs, axis=-1, keepdims=True) + 1e-06)
    xs = (xs * rs2 * gain2[...]).astype(BF16)
    gate = mm(xs, wgu[pl.ds(0, hid)], NT)
    up = mm(xs, wgu[pl.ds(hid, hid)], NT)
    hidden = (gate / (1.0 + jnp.exp(-gate)) * up).astype(BF16)
    c_wd.wait()
    part = mm(hidden, wd[...]).astype(BF16)
    piled = []
    for k in range(2):
        piled.append(jnp.concatenate([
            jnp.concatenate([part[:, (2 * (j * per + v) + k) * slc:][:, :slc] for v in range(per)], axis=1)
            for j in range(parts)], axis=0))
    for k in range(2):
        es[pl.ds(k * ne, ne)] = mm(spread[...], piled[k]).astype(BF16).reshape(ne, 16, cw)
    send_chips(es, er, 6, True)
    er[core * ne + g] = es[core * ne + g]
    arrived(er, 6)
    both = (mm(comb[...], er[pl.ds(0, ne)].reshape(lanes, cw))
            + mm(comb[...], er[pl.ds(ne, ne)].reshape(lanes, cw)))
    for j in range(parts):
        piece = (both[2 * j * seqs:(2 * j + 1) * seqs] + both[(2 * j + 1) * seqs:(2 * j + 2) * seqs]).astype(BF16)
        for u in range(per):
            fs[j * per + u] = piece[:, u * slc:(u + 1) * slc]
    send_z(fs, fr, 7)
    fr[z] = fs[z]
    arrived(fr, 7)
    out_ref[...] = (mixed.astype(F32) + jnp.sum(fr[...].astype(F32), axis=0)).astype(BF16)

    for phase, buf in enumerate((xin, qr, kvr, or_, mxr, sr, er, fr)):
        gone(buf, phase)


def shards(
    ne, nt, stream, norm_gain_attn, w_query, w_key, w_value, w_forget, forget_bias,
    key_cache, value_cache, gate_cache, lengths, w_output, norm_gain_ffn,
    routes, route_weights, w_expert_gate, w_expert_up, expert_down_weight,
):
    seqs, width = stream.shape
    cache, hd = key_cache.shape[1:]
    tops = routes.shape[1]
    cap = 2 * seqs * tops // ne
    blk, slc, hid = width // ne, width // nt, w_expert_gate.shape[2]
    parts = 16 // cap
    cw = width // 2 // parts
    args = (
        stream, norm_gain_attn.reshape(1, -1), w_query, w_key, w_value, w_forget.T,
        forget_bias.reshape(1, -1), key_cache, value_cache, gate_cache, lengths.reshape(1, -1),
        w_output, norm_gain_ffn.reshape(1, -1), routes.T, route_weights.T,
        jnp.swapaxes(w_expert_gate, 1, 2), jnp.swapaxes(w_expert_up, 1, 2), expert_down_weight,
    )
    V = pltpu.VMEM
    scratch = [
        V((seqs, width), BF16), V((1, width), F32), V((blk, 3 * hd), BF16),
        V(w_forget.shape[::-1], BF16), V((1, forget_bias.shape[0]), F32),
        V(key_cache.shape, BF16), V(value_cache.shape, BF16), V(gate_cache.shape, F32),
        V((1, seqs), jnp.int32), V(w_output.shape, BF16), V((1, width), F32),
        V(routes.shape[::-1], jnp.int32), V(routes.shape[::-1], F32),
        V((2 * hid, width), BF16), V((hid, width), BF16),
        V((ne, seqs, blk), BF16), V((ne, seqs, blk), BF16),
        V((ne, seqs, hd), F32), V((ne, seqs, 2 * hd), BF16),
        V((ne, seqs, hd), F32), V((ne, seqs, 2 * hd), BF16),
        V((nt, seqs, slc), BF16), V((nt, seqs, slc), BF16),
        V((seqs, slc), BF16), V((nt // 2, seqs, slc), BF16),
        V((ne, 16, cw), BF16), V((2 * ne, 16, cw), BF16),
        V((2 * ne, 16, cw), BF16), V((2 * ne, 16, cw), BF16),
        V((nt // 2, seqs, slc), BF16), V((nt // 2, seqs, slc), BF16),
        V((ne * 16, parts * seqs), BF16), V((parts * ne * cap, ne * 16), BF16),
        V((ne * 16, parts * ne * cap), BF16), V((2 * parts * seqs, ne * 16), BF16),
        pltpu.SemaphoreType.DMA((18,)), pltpu.SemaphoreType.DMA((8,)), pltpu.SemaphoreType.DMA((8,)),
    ]
    return pl.pallas_call(
        functools.partial(kernel, (ne, nt, cap)),
        out_shape=jax.ShapeDtypeStruct((seqs, slc), BF16),
        in_specs=[pl.BlockSpec(memory_space=pltpu.HBM)] * len(args),
        out_specs=pl.BlockSpec(memory_space=pltpu.VMEM),
        scratch_shapes=scratch,
        compiler_params=pltpu.CompilerParams(
            collective_id=0, has_side_effects=True, vmem_limit_bytes=67043328),
        name="layer",
    )(*args)


def solution(mesh):
    placed = (
        P("ep", None), P(), P("ep", "tp"), P("ep", "tp"), P("ep", "tp"), P(), P(),
        P("ep", None, "tp"), P("ep", None, "tp"), P("ep", "tp", None), P("ep"),
        P("tp", None), P(), P(), P(),
        P("ep", None, "tp"), P("ep", None, "tp"), P("ep", "tp", None),
    )
    return jax.shard_map(
        functools.partial(shards, mesh.shape["ep"], mesh.shape["tp"]),
        mesh=mesh, in_specs=placed, out_specs=P("ep", "tp"), check_vma=False,
    )
```
